32 devices in a mesh: sp: 4 (over y, x), dp: 8 (over z, core).
Axes of the slice: x: 2, y: 2, z: 4, core: 2. Of those that a mesh axis runs over, the one named last changes fastest.
Arguments:
- tokens: bfloat16 [8, 1024, 2048], P('dp', 'sp'), may hold values from -6 to 6
- in_gain: float32 [2048], replicated, may hold values from 0.1 to 1.9
- query_weight: bfloat16 [2048, 2048], P('dp'), may hold values from -1 to 1
- key_weight: bfloat16 [2048, 512], P('dp'), may hold values from -1 to 1
- value_matrix: bfloat16 [2048, 512], P('dp'), may hold values from -0.125 to 0.125
- query_gain: float32 [128], replicated, may hold values from 1 to 6
- key_gain: float32 [128], replicated, may hold values from 1 to 6
- out_weight: bfloat16 [2048, 2048], P('dp'), may hold values from -0.125 to 0.125
- out_gain: float32 [2048], replicated, may hold values from 0.1 to 1.9
Outputs:
- mixed: bfloat16 [8, 1024, 2048], P('dp', 'sp')
The draws below stay inside these ranges and needn't reach their ends.
All inputs are finite; a program needn't handle non-finite values.
Results may differ from the reference program's by a relative error of at most 0.0055.
The reference program's roundings to bfloat16 on the way count: a program that leaves them out, or rounds other values in their place, can miss the bound.
Values may be sent and summed in bfloat16 or wider, within the bound.
No kernel may reach another device: no remote copies, remote signals or barrier semaphores. Data moves between devices by JAX's collectives and lax.ppermute only.
A program may use at most 128 MiB of HBM per device.

```python
import jax
import jax.numpy as jnp
from jax import lax

MODEL_WIDTH = 2048
QUERY_HEAD_COUNT = 16
KEY_VALUE_HEADS = 4
HEAD_WIDTH = 128
GRID_W = 64
SEQUENCE_LENGTH = 1024
BATCH = 8


def query_for_group(key):
    return jax.random.truncated_normal(jax.random.fold_in(key, 101), -6.0, 6.0, (MODEL_WIDTH, QUERY_HEAD_COUNT * HEAD_WIDTH), jnp.float32) * MODEL_WIDTH ** (-0.5)


def draw_query_weight(key, part):
    return query_for_group(key).astype(jnp.bfloat16)


def draw_key_weight(key, part):
    complete_output = jax.random.truncated_normal(jax.random.fold_in(key, 401), -6.0, 6.0, (MODEL_WIDTH, KEY_VALUE_HEADS * HEAD_WIDTH), jnp.float32) * MODEL_WIDTH ** (-0.5)
    return complete_output.astype(jnp.bfloat16)


def draw_query_gain(key, part):
    return 1.6 * (1.0 + 0.18 * jax.random.uniform(jax.random.fold_in(key, 201), (HEAD_WIDTH,), jnp.float32, -1.0, 1.0))


def draw_key_gain(key, part):
    return 1.6 * (1.0 + 0.18 * jax.random.uniform(jax.random.fold_in(key, 301), (HEAD_WIDTH,), jnp.float32, -1.0, 1.0))


def level_of(key, dims, split, low, largest):
    def one(dim, shards_of):
        heights = jax.random.uniform(jax.random.fold_in(jax.random.fold_in(key, 6), dim), (shards_of,), jnp.float32, low / len(split), largest / len(split))
        return jnp.repeat(jnp.exp(heights), dims[dim] // shards_of).reshape((-1,) + (1,) * (len(dims) - dim - 1))

    level = one(*split[0])
    for cut in split[1:]:
        level = level * one(*cut)
    return level


def gaussian(rng, extent, deviation, reach, pieces=(), kind=jnp.bfloat16):
    drawn = deviation * jax.random.normal(rng, extent, jnp.float32)
    if pieces:
        drawn = drawn * level_of(rng, extent, pieces, -0.22, 0.18)
    return jnp.clip(drawn, -reach, reach).astype(kind)


def setup_inputs(seed: int = 0) -> dict:
    seeds = jax.random.split(jax.random.key(seed), 10)
    return {
        "tokens": gaussian(seeds[0], (BATCH, SEQUENCE_LENGTH, MODEL_WIDTH), 1.0, 6.0, ((0, 8), (1, 4))),
        "in_gain": jnp.clip(1.0 + 0.18 * jax.random.normal(seeds[1], (MODEL_WIDTH,), jnp.float32), 0.1, 1.9),
        "query_weight": draw_query_weight(jax.random.fold_in(seeds[9], 71), 0),
        "key_weight": draw_key_weight(jax.random.fold_in(seeds[9], 71), 0),
        "value_matrix": gaussian(seeds[4], (MODEL_WIDTH, KEY_VALUE_HEADS * HEAD_WIDTH), MODEL_WIDTH ** -0.5, 0.125, ((0, 8),)),
        "query_gain": draw_query_gain(jax.random.fold_in(seeds[9], 71), 0),
        "key_gain": draw_key_gain(jax.random.fold_in(seeds[9], 71), 0),
        "out_weight": gaussian(seeds[7], (QUERY_HEAD_COUNT * HEAD_WIDTH, MODEL_WIDTH), (QUERY_HEAD_COUNT * HEAD_WIDTH) ** -0.5, 0.125, ((0, 8),)),
        "out_gain": jnp.clip(1.0 + 0.18 * jax.random.normal(seeds[8], (MODEL_WIDTH,), jnp.float32), 0.1, 1.9),
    }


EPS = 1e-06
THETA = 10000.0

def norm_rows(row_data, gain_vec):
    return row_data * lax.rsqrt(lax.optimization_barrier(jnp.mean(row_data * row_data, axis=-1, keepdims=True)) + EPS) * gain_vec.astype(jnp.float32)

def rotate(head_data, positions):
    head_size = head_data.shape[-1]
    half_size = head_size // 2
    quarter = head_size // 4
    inverse_freq = THETA ** (-jnp.arange(quarter, dtype=jnp.float32) / quarter)
    row_angle = (positions // GRID_W).astype(jnp.float32)[:, None] * inverse_freq[None, :]
    col_angle = (positions % GRID_W).astype(jnp.float32)[:, None] * inverse_freq[None, :]

    def turn_half(half_part, angle):
        cosine = jnp.cos(angle)[:, None, :]
        sine_val = jnp.sin(angle)[:, None, :]
        first_part = half_part[..., :quarter]
        second_part = half_part[..., quarter:]
        return jnp.concatenate([first_part * cosine - second_part * sine_val, second_part * cosine + first_part * sine_val], axis=-1)
    return jnp.concatenate([turn_half(head_data[..., :half_size], row_angle), turn_half(head_data[..., half_size:], col_angle)], axis=-1)

def finish(projected, gain_vec, positions):
    row_count = projected.shape[0]
    heads_data = projected.reshape(row_count, -1, HEAD_WIDTH)
    heads_data = rotate(norm_rows(heads_data, gain_vec), positions)
    return heads_data.reshape(row_count, -1).astype(jnp.bfloat16)

def reference(tokens, in_gain, query_weight, key_weight, value_matrix, query_gain, key_gain, out_weight, out_gain):
    queries_per_group = QUERY_HEAD_COUNT // KEY_VALUE_HEADS
    rows_per_block = min(512, SEQUENCE_LENGTH)

    def per_sequence(sequence):
        float_rows = sequence.astype(jnp.float32)
        normed = norm_rows(float_rows, in_gain).astype(jnp.bfloat16)
        positions = jnp.arange(SEQUENCE_LENGTH, dtype=jnp.int32)
        query_rows = finish(jnp.dot(normed, query_weight, preferred_element_type=jnp.float32), query_gain, positions)
        key_matrix_rows = finish(jnp.dot(normed, key_weight, preferred_element_type=jnp.float32), key_gain, positions)
        value_rows = jnp.dot(normed, value_matrix, preferred_element_type=jnp.float32).astype(jnp.bfloat16)
        key_rows_float = key_matrix_rows.reshape(SEQUENCE_LENGTH, KEY_VALUE_HEADS, HEAD_WIDTH).astype(jnp.float32)
        value_rows_float = value_rows.reshape(SEQUENCE_LENGTH, KEY_VALUE_HEADS, HEAD_WIDTH).astype(jnp.float32)
        query_block_list = query_rows.reshape(SEQUENCE_LENGTH // rows_per_block, rows_per_block, KEY_VALUE_HEADS, queries_per_group, HEAD_WIDTH)

        def attend(query_block):
            scores = jnp.einsum('qegd,ked->egqk', query_block.astype(jnp.float32), key_rows_float) * HEAD_WIDTH ** (-0.5)
            shifted = scores - lax.optimization_barrier(jnp.max(scores, axis=-1, keepdims=True))
            raised = jnp.exp(shifted)
            weights = (raised / lax.optimization_barrier(jnp.sum(raised, axis=-1, keepdims=True))).astype(jnp.bfloat16)
            attended = jnp.einsum('egqk,ked->qegd', weights.astype(jnp.float32), value_rows_float)
            return attended.astype(jnp.bfloat16)
        attended = lax.map(attend, query_block_list).reshape(SEQUENCE_LENGTH, QUERY_HEAD_COUNT * HEAD_WIDTH)
        projected = jnp.dot(attended, out_weight, preferred_element_type=jnp.float32)
        return norm_rows(projected, out_gain).astype(jnp.bfloat16)
    return lax.map(per_sequence, tokens)
```

```python
import functools
import math

import jax
import jax.numpy as jnp
import numpy as np
from jax import lax
from jax.experimental import pallas as pl
from jax.experimental.pallas import tpu as pltpu
from jax.sharding import PartitionSpec as P

QUERY_HEAD_COUNT = 16
KEY_VALUE_HEADS = 4
HEAD_WIDTH = 128
GRID_W = 64

EPS = 1e-06
THETA = 10000.0
VMEM_BYTES = 56 * 1024 * 1024


ANY = pl.BlockSpec(memory_space=pl.ANY)
SMEM = pl.BlockSpec(memory_space=pltpu.SMEM)


def call(kernel, outs, scratch, n_in, name, flops, specs=None, out_specs=None):
    return pl.pallas_call(
        kernel,
        out_shape=outs,
        in_specs=specs or [SMEM] + [ANY] * n_in,
        out_specs=out_specs or jax.tree.map(lambda _: pl.BlockSpec(memory_space=pltpu.VMEM), outs),
        scratch_shapes=scratch,
        name=name,
        compiler_params=pltpu.CompilerParams(vmem_limit_bytes=VMEM_BYTES),
        cost_estimate=pl.CostEstimate(flops=flops, bytes_accessed=1 << 20, transcendentals=0),
    )


def orders(size):
    bits = [1 << i for i in range(size.bit_length() - 1)]
    turn = len(bits) // 2
    return bits, bits[turn:] + bits[:turn]


def offsets(size):
    out = []
    for order in orders(size):
        out.append([functools.reduce(lambda a, b: a ^ b, [o for i, o in enumerate(order) if j >> i & 1], 0) for j in range(size)])
    return out


def plane_swap(value, even, odd):
    sp, dp = lax.axis_size("sp"), lax.axis_size("dp")
    pairs = []
    for s in range(sp):
        for d in range(dp):
            pairs.append((s * dp + d, (s ^ (odd if d % 2 else even)) * dp + d))
    return lax.ppermute(value, ("sp", "dp"), pairs)


def plane_gather(value):
    blocks = [value]
    even, odd = orders(lax.axis_size("sp"))
    for a, b in zip(even, odd):
        blocks = blocks + [plane_swap(block, a, b) for block in blocks]
    return blocks


def line_swap(value, bit):
    return lax.ppermute(value, "dp", [(d, d ^ bit) for d in range(lax.axis_size("dp"))])


def line_gather(value, bits):
    blocks, rel = [value], [0]
    for bit in bits:
        blocks = blocks + [line_swap(block, bit) for block in blocks]
        rel = rel + [r ^ bit for r in rel]
    return blocks, rel


def prepare_kernel(widths, place, tokens, gain, qw, kw, vw, ow, normed, cols, quarter, sems):
    q_width, kv_width, o_width = widths
    q_at = pl.multiple_of(place[0] * q_width, 128)
    kv_at = pl.multiple_of(place[1] * HEAD_WIDTH, 128)
    o_at = pl.multiple_of(place[0] * o_width, 128)
    copies = [
        pltpu.make_async_copy(qw.at[:, pl.ds(q_at, q_width)], cols.at[:, pl.ds(0, q_width)], sems.at[0]),
        pltpu.make_async_copy(kw.at[:, pl.ds(kv_at, kv_width)], cols.at[:, pl.ds(q_width, kv_width)], sems.at[1]),
        pltpu.make_async_copy(vw.at[:, pl.ds(kv_at, kv_width)], cols.at[:, pl.ds(q_width + kv_width, kv_width)], sems.at[2]),
        pltpu.make_async_copy(ow.at[:, pl.ds(o_at, o_width)], quarter, sems.at[3]),
    ]
    for copy in copies:
        copy.start()
    rows = tokens[...].astype(jnp.float32)
    scale = lax.rsqrt(jnp.mean(rows * rows, axis=-1, keepdims=True) + EPS)
    normed[...] = (rows * scale * gain[...]).astype(jnp.bfloat16)
    for copy in copies:
        copy.wait()


def project_kernel(shape, rel, place, *refs):
    n_blocks, heads, kv = shape
    n_w = len(rel)
    xs, ws = refs[:n_blocks], refs[n_blocks : n_blocks + n_w]
    table, gains = refs[n_blocks + n_w : n_blocks + n_w + 2]
    outs = refs[n_blocks + n_w + 2 : 2 * n_blocks + n_w + 2]
    x_buf, w_buf, t_buf, x_sem, w_sem, t_sem = refs[2 * n_blocks + n_w + 2 :]
    rows, w_rows = xs[0].shape[0], ws[0].shape[0]
    w_copies = []
    for j in range(n_w):
        at = pl.multiple_of((place[0] ^ rel[j]) * w_rows, w_rows)
        w_copies.append(pltpu.make_async_copy(ws[j], w_buf.at[pl.ds(at, w_rows)], w_sem.at[j]))
    x_copies, t_copies = [], []
    for i in range(n_blocks):
        at = pl.multiple_of(place[1 + i] * rows, rows)
        x_copies.append(pltpu.make_async_copy(xs[i], x_buf.at[i], x_sem.at[i]))
        t_copies.append(pltpu.make_async_copy(table.at[pl.ds(at, rows)], t_buf.at[i], t_sem.at[i]))
    x_copies[0].start()
    for copy in w_copies:
        copy.start()
    for copy in x_copies[1:] + t_copies:
        copy.start()
    for copy in w_copies:
        copy.wait()
    lane = lax.broadcasted_iota(jnp.int32, (rows, HEAD_WIDTH), 1)
    low = lane % (HEAD_WIDTH // 2) < HEAD_WIDTH // 4
    for i in range(n_blocks):
        x_copies[i].wait()
        t_copies[i].wait()
        blended = jnp.dot(x_buf[i], w_buf[...], preferred_element_type=jnp.float32)
        cosine, sine = t_buf[i, :, :HEAD_WIDTH], t_buf[i, :, HEAD_WIDTH:]
        for h in range(heads + kv):
            part = blended[:, h * HEAD_WIDTH : (h + 1) * HEAD_WIDTH]
            gain = gains[0:1, :] if h < heads else gains[1:2, :]
            scale = lax.rsqrt(jnp.mean(part * part, axis=-1, keepdims=True) + EPS)
            part = part * scale * gain
            other = jnp.where(
                low,
                pltpu.roll(part, HEAD_WIDTH - HEAD_WIDTH // 4, 1),
                pltpu.roll(part, HEAD_WIDTH // 4, 1),
            )
            outs[i][:, h * HEAD_WIDTH : (h + 1) * HEAD_WIDTH] = (part * cosine + other * sine).astype(jnp.bfloat16)
        outs[i][:, (heads + kv) * HEAD_WIDTH :] = blended[:, (heads + kv) * HEAD_WIDTH :].astype(jnp.bfloat16)


def attend_kernel(shape, place, *refs):
    n_blocks, which, heads, kv = shape
    blocks = refs[:n_blocks]
    out = refs[n_blocks]
    q_buf, kv_buf, q_sem, kv_sem = refs[n_blocks + 1 :]
    rows = blocks[0].shape[0]
    q_copy = pltpu.make_async_copy(blocks[which].at[:, pl.ds(0, heads * HEAD_WIDTH)], q_buf, q_sem)
    q_copy.start()
    copies = []
    for j in range(n_blocks):
        copy = pltpu.make_async_copy(
            blocks[j].at[:, pl.ds(heads * HEAD_WIDTH, 2 * kv * HEAD_WIDTH)], kv_buf.at[pl.ds(j * rows, rows)], kv_sem.at[j]
        )
        copy.start()
        copies.append(copy)
    q_copy.wait()
    for copy in copies:
        copy.wait()
    factor = HEAD_WIDTH ** (-0.5) * math.log2(math.e)
    for h in range(heads):
        e = h * kv // heads
        keys = kv_buf[:, e * HEAD_WIDTH : (e + 1) * HEAD_WIDTH]
        values = kv_buf[:, (kv + e) * HEAD_WIDTH : (kv + e + 1) * HEAD_WIDTH]
        query = q_buf[:, h * HEAD_WIDTH : (h + 1) * HEAD_WIDTH]
        scores = lax.dot_general(query, keys, (((1,), (1,)), ((), ())), preferred_element_type=jnp.float32)
        shifted = (scores - jnp.max(scores, axis=-1, keepdims=True)) * factor
        raised = jnp.exp2(shifted)
        weights = (raised * (1.0 / jnp.sum(raised, axis=-1, keepdims=True))).astype(jnp.bfloat16)
        attended = jnp.dot(weights, values, preferred_element_type=jnp.float32)
        out[:, h * HEAD_WIDTH : (h + 1) * HEAD_WIDTH] = attended.astype(jnp.bfloat16)


def finish_kernel(shape, place, *refs):
    n_heads, n_pieces = shape
    heads, pieces = refs[:n_heads], refs[n_heads : n_heads + n_pieces]
    gain, out = refs[n_heads + n_pieces : n_heads + n_pieces + 2]
    a_buf, w_buf, a_sem, w_sem = refs[n_heads + n_pieces + 2 :]
    copies = []
    for j in range(n_heads):
        width = heads[j].shape[1]
        at = pl.multiple_of(place[j] * width, width)
        copies.append(pltpu.make_async_copy(heads[j], a_buf.at[:, pl.ds(at, width)], a_sem.at[j]))
    for j in range(n_pieces):
        height, width = pieces[j].shape
        row = pl.multiple_of(place[n_heads + 2 * j] * height, height)
        col = pl.multiple_of(place[n_heads + 2 * j + 1] * width, width)
        copies.append(pltpu.make_async_copy(pieces[j], w_buf.at[pl.ds(row, height), pl.ds(col, width)], w_sem.at[j]))
    for copy in copies:
        copy.start()
    for copy in copies:
        copy.wait()
    projected = jnp.dot(a_buf[...], w_buf[...], preferred_element_type=jnp.float32)
    scale = lax.rsqrt(jnp.mean(projected * projected, axis=-1, keepdims=True) + EPS)
    out[...] = (projected * scale * gain[...]).astype(jnp.bfloat16)


def rotation_table(length):
    quarter = HEAD_WIDTH // 4
    freq = THETA ** (-np.arange(quarter) / quarter)
    at = np.arange(length)
    row, col = (at // GRID_W)[:, None] * freq, (at % GRID_W)[:, None] * freq
    cosine = [np.cos(row), np.cos(row), np.cos(col), np.cos(col)]
    sine = [-np.sin(row), np.sin(row), -np.sin(col), np.sin(col)]
    return jnp.asarray(np.concatenate(cosine + sine, axis=1).astype(np.float32))


def on_device(tokens, in_gain, query_weight, key_weight, value_matrix, query_gain, key_gain, out_weight, out_gain):
    sequence = tokens[0]
    sp, dp = lax.axis_size("sp"), lax.axis_size("dp")
    s, d = lax.axis_index("sp"), lax.axis_index("dp")
    odd = d % 2 == 1
    rows, width = sequence.shape
    w_rows = query_weight.shape[0]
    heads = QUERY_HEAD_COUNT // sp
    kv = max(1, KEY_VALUE_HEADS // sp)
    first_kv = s * heads // (QUERY_HEAD_COUNT // KEY_VALUE_HEADS)
    q_width, kv_width, o_width = heads * HEAD_WIDTH, kv * HEAD_WIDTH, out_weight.shape[1] // sp
    all_width = q_width + 2 * kv_width
    bf16 = jnp.bfloat16
    dma = pltpu.SemaphoreType.DMA

    whole = pl.BlockSpec(memory_space=pltpu.VMEM)
    normed, cols, quarter = call(
        functools.partial(prepare_kernel, (q_width, kv_width, o_width)),
        (
            jax.ShapeDtypeStruct((rows, width), bf16),
            jax.ShapeDtypeStruct((w_rows, all_width), bf16),
            jax.ShapeDtypeStruct((w_rows, o_width), bf16),
        ),
        [dma((4,))],
        6,
        "prepare",
        rows * width * 10,
        specs=[SMEM, whole, whole, ANY, ANY, ANY, ANY],
        out_specs=(whole, ANY, ANY),
    )(
        jnp.stack([s, first_kv]).astype(jnp.int32),
        sequence,
        in_gain.reshape(1, -1),
        query_weight,
        key_weight,
        value_matrix,
        out_weight,
    )

    even_rel, odd_rel = offsets(sp)
    source = [s ^ jnp.where(odd, o, e) for e, o in zip(even_rel, odd_rel)]
    partner = [s ^ jnp.where(odd, e, o) for e, o in zip(even_rel, odd_rel)]
    line_bits = [1 << i for i in range(dp.bit_length() - 2, -1, -1)]
    x_blocks = plane_gather(normed)
    w_blocks, w_rel = line_gather(cols, line_bits)

    if sp * dp > 64:
        pieces = [(lax.all_gather(out_weight, "dp", axis=0, tiled=True), 0 * d, 0 * d)]
    else:
        pieces = [(out_weight, d, 0 * d), (line_swap(out_weight, 1), d ^ 1, 0 * d)]
        z_blocks, z_rel = line_gather(quarter, line_bits[:-1])
        for block, rel in list(zip(z_blocks, z_rel))[1:]:
            for j, piece in enumerate(plane_gather(block)):
                pieces.append((piece, d ^ rel, source[j]))
                pieces.append((line_swap(piece, 1), d ^ rel ^ 1, partner[j]))

    table = rotation_table(rows * sp)
    gains = jnp.stack([query_gain, key_gain])
    blocks = []
    cut = sp // 2 + 1
    for group in (range(0, cut), range(cut, sp)):
        n = len(group)
        if not n:
            continue
        blocks += call(
            functools.partial(project_kernel, (n, heads, kv), w_rel),
            tuple(jax.ShapeDtypeStruct((rows, all_width), bf16) for _ in group),
            [
                pltpu.VMEM((n, rows, width), bf16),
                pltpu.VMEM((width, all_width), bf16),
                pltpu.VMEM((n, rows, 2 * HEAD_WIDTH), jnp.float32),
                dma((n,)),
                dma((dp,)),
                dma((n,)),
            ],
            None,
            "project",
            2 * n * rows * width * all_width,
            specs=[SMEM] + [ANY] * (n + dp + 1) + [whole],
        )(
            jnp.stack([d] + [source[j] for j in group]).astype(jnp.int32),
            *[x_blocks[j] for j in group],
            *w_blocks,
            table,
            gains,
        )

    returned = []
    for j in [*range(1, sp)][::-1] + [0]:
        attended = call(
            functools.partial(attend_kernel, (sp, j, heads, kv)),
            jax.ShapeDtypeStruct((rows, q_width), bf16),
            [
                pltpu.VMEM((rows, q_width), bf16),
                pltpu.VMEM((rows * sp, 2 * kv_width), bf16),
                dma,
                dma((sp,)),
            ],
            sp,
            "attend",
            4 * rows * rows * sp * q_width,
        )(jnp.zeros((1,), jnp.int32), *blocks)
        if j:
            attended = plane_swap(attended, even_rel[j], odd_rel[j])
        returned.append((attended, source[j]))

    place = [c for _, c in returned]
    for _, r, c in pieces:
        place += [r, c]
    result = call(
        functools.partial(finish_kernel, (sp, len(pieces))),
        jax.ShapeDtypeStruct((rows, width), bf16),
        [
            pltpu.VMEM((rows, q_width * sp), bf16),
            pltpu.VMEM((q_width * sp, width), bf16),
            dma((sp,)),
            dma((len(pieces),)),
        ],
        None,
        "finish",
        2 * rows * width * width,
        specs=[SMEM] + [ANY] * (sp + len(pieces)) + [whole],
    )(
        jnp.stack(place).astype(jnp.int32),
        *[a for a, _ in returned],
        *[p for p, _, _ in pieces],
        out_gain.reshape(1, -1),
    )
    return result[None]


def solution(mesh):
    placed = (
        P("dp", "sp", None),
        P(),
        P("dp", None),
        P("dp", None),
        P("dp", None),
        P(),
        P(),
        P("dp", None),
        P(),
    )
    return jax.shard_map(on_device, mesh=mesh, in_specs=placed, out_specs=P("dp", "sp", None), check_vma=False)
```

```python
import functools
import math

import jax
import jax.numpy as jnp
import numpy as np
from jax import lax
from jax.experimental import pallas as pl
from jax.experimental.pallas import tpu as pltpu
from jax.sharding import PartitionSpec as P

QUERY_HEAD_COUNT = 16
KEY_VALUE_HEADS = 4
HEAD_WIDTH = 128
GRID_W = 64

EPS = 1e-06
THETA = 10000.0

ANY = pl.BlockSpec(memory_space=pl.ANY)
VMEM = pl.BlockSpec(memory_space=pltpu.VMEM)
DMA = pltpu.SemaphoreType.DMA
BF16 = jnp.bfloat16
MIB = 1 << 20


def call(kernel, name, args, specs, outs, scratch, flops, mib):
    outs = tuple(jax.ShapeDtypeStruct(shape, BF16) for shape in outs)
    return pl.pallas_call(
        kernel,
        out_shape=outs,
        in_specs=specs,
        out_specs=tuple(VMEM for _ in outs),
        scratch_shapes=scratch,
        name=name,
        compiler_params=pltpu.CompilerParams(vmem_limit_bytes=mib * MIB),
        cost_estimate=pl.CostEstimate(flops=flops, bytes_accessed=MIB, transcendentals=0),
    )(*args)


def orders(size):
    bits = [1 << i for i in range(size.bit_length() - 1)]
    turn = len(bits) // 2
    return bits, bits[turn:] + bits[:turn]


def offsets(size):
    out = []
    for order in orders(size):
        out.append([functools.reduce(lambda a, b: a ^ b, [o for i, o in enumerate(order) if j >> i & 1], 0) for j in range(size)])
    return out


def plane_swap(value, even, odd):
    sp, dp = lax.axis_size("sp"), lax.axis_size("dp")
    pairs = []
    for s in range(sp):
        for d in range(dp):
            pairs.append((s * dp + d, (s ^ (odd if d % 2 else even)) * dp + d))
    return lax.ppermute(value, ("sp", "dp"), pairs)


def plane_gather(value):
    blocks = [value]
    even, odd = orders(lax.axis_size("sp"))
    for a, b in zip(even, odd):
        blocks = blocks + [plane_swap(block, a, b) for block in blocks]
    return blocks


def line_swap(value, bit):
    return lax.ppermute(value, "dp", [(d, d ^ bit) for d in range(lax.axis_size("dp"))])


def line_gather(value, bits):
    blocks, rel = [value], [0]
    for bit in bits:
        blocks = blocks + [line_swap(block, bit) for block in blocks]
        rel = rel + [r ^ bit for r in rel]
    return blocks, rel


def rank_of(rel, flip=0):
    odd = (lax.axis_index("dp") + flip) % 2 == 1
    return lax.axis_index("sp") ^ jnp.where(odd, rel[1], rel[0])


def prepare_kernel(widths, tokens, gain, qw, kw, vw, ow, normed, cols, quarter, sems):
    q_width, kv_width, o_width, per_kv = widths
    s = lax.axis_index("sp")
    q_at = pl.multiple_of(s * q_width, 128)
    kv_at = pl.multiple_of(s * (q_width // HEAD_WIDTH) // per_kv * HEAD_WIDTH, 128)
    o_at = pl.multiple_of(s * o_width, 128)
    copies = [
        pltpu.make_async_copy(qw.at[:, pl.ds(q_at, q_width)], cols.at[:, pl.ds(0, q_width)], sems.at[0]),
        pltpu.make_async_copy(kw.at[:, pl.ds(kv_at, kv_width)], cols.at[:, pl.ds(q_width, kv_width)], sems.at[1]),
        pltpu.make_async_copy(vw.at[:, pl.ds(kv_at, kv_width)], cols.at[:, pl.ds(q_width + kv_width, kv_width)], sems.at[2]),
        pltpu.make_async_copy(ow.at[:, pl.ds(o_at, o_width)], quarter, sems.at[3]),
    ]
    for copy in copies:
        copy.start()
    rows = tokens[...].astype(jnp.float32)
    scale = lax.rsqrt(jnp.mean(rows * rows, axis=-1, keepdims=True) + EPS)
    normed[...] = (rows * scale * gain[...]).astype(BF16)
    for copy in copies:
        copy.wait()


def project_blocks(heads, kv, weight, xs, rels, table, gains, q_outs, kv_outs, t_buf, t_sem):
    rows = xs[0].shape[0]
    copies = []
    for i, rel in enumerate(rels):
        at = pl.multiple_of(rank_of(rel) * rows, rows)
        copies.append(pltpu.make_async_copy(table.at[pl.ds(at, rows)], t_buf.at[i], t_sem.at[i]))
        copies[-1].start()
    yield
    lane = lax.broadcasted_iota(jnp.int32, (rows, HEAD_WIDTH), 1)
    low = lane % (HEAD_WIDTH // 2) < HEAD_WIDTH // 4
    for i, x in enumerate(xs):
        copies[i].wait()
        blended = jnp.dot(x[...], weight[...], preferred_element_type=jnp.float32)
        cosine, sine = t_buf[i, :, :HEAD_WIDTH], t_buf[i, :, HEAD_WIDTH:]
        for h in range(heads + kv):
            part = blended[:, h * HEAD_WIDTH : (h + 1) * HEAD_WIDTH]
            gain = gains[0:1, :] if h < heads else gains[1:2, :]
            scale = lax.rsqrt(jnp.mean(part * part, axis=-1, keepdims=True) + EPS)
            part = part * scale * gain
            other = jnp.where(
                low,
                pltpu.roll(part, HEAD_WIDTH - HEAD_WIDTH // 4, 1),
                pltpu.roll(part, HEAD_WIDTH // 4, 1),
            )
            turned = (part * cosine + other * sine).astype(BF16)
            if h < heads:
                q_outs[i][:, h * HEAD_WIDTH : (h + 1) * HEAD_WIDTH] = turned
            else:
                kv_outs[i][:, (h - heads) * HEAD_WIDTH : (h - heads + 1) * HEAD_WIDTH] = turned
        kv_outs[i][:, kv * HEAD_WIDTH :] = blended[:, (heads + kv) * HEAD_WIDTH :].astype(BF16)
    yield


def project_first_kernel(heads, kv, rels, w_rel, *refs):
    n, n_w = len(rels), len(w_rel)
    xs, ws, (table, gains) = refs[:n], refs[n : n + n_w], refs[n + n_w : n + n_w + 2]
    outs = refs[n + n_w + 2 :]
    weight, t_buf, w_sem, t_sem = outs[2 * n :]
    w_rows = ws[0].shape[0]
    copies = []
    for j in range(n_w):
        at = pl.multiple_of((lax.axis_index("dp") ^ w_rel[j]) * w_rows, w_rows)
        copies.append(pltpu.make_async_copy(ws[j], weight.at[pl.ds(at, w_rows)], w_sem.at[j]))
        copies[-1].start()
    steps = project_blocks(heads, kv, weight, xs, rels, table, gains, outs[:n], outs[n : 2 * n], t_buf, t_sem)
    next(steps)
    for copy in copies:
        copy.wait()
    next(steps)


def project_rest_kernel(heads, kv, rels, *refs):
    n = len(rels)
    xs, (weight, table, gains), outs = refs[:n], refs[n : n + 3], refs[n + 3 :]
    t_buf, t_sem = outs[2 * n :]
    for _ in project_blocks(heads, kv, weight, xs, rels, table, gains, outs[:n], outs[n : 2 * n], t_buf, t_sem):
        pass


def attend_kernel(n_q, n_kv, heads, kv, *refs):
    qs, kvs, outs, kv_buf = refs[:n_q], refs[n_q : n_q + n_kv], refs[n_q + n_kv : 2 * n_q + n_kv], refs[-1]
    rows = qs[0].shape[0]
    for j in range(n_kv):
        kv_buf[j * rows : (j + 1) * rows, :] = kvs[j][...]
    factor = HEAD_WIDTH ** (-0.5) * math.log2(math.e)
    items = [(j, h) for j in range(n_q) for h in range(heads)]

    def score(item):
        j, h = item
        e = h * kv // heads
        keys = kv_buf[:, e * HEAD_WIDTH : (e + 1) * HEAD_WIDTH]
        query = qs[j][:, h * HEAD_WIDTH : (h + 1) * HEAD_WIDTH]
        return lax.dot_general(query, keys, (((1,), (1,)), ((), ())), preferred_element_type=jnp.float32)

    scores = score(items[0])
    for i, (j, h) in enumerate(items):
        following = score(items[i + 1]) if i + 1 < len(items) else None
        e = h * kv // heads
        values = kv_buf[:, (kv + e) * HEAD_WIDTH : (kv + e + 1) * HEAD_WIDTH]
        raised = jnp.exp2((scores - jnp.max(scores, axis=-1, keepdims=True)) * factor)
        weights = (raised * (1.0 / jnp.sum(raised, axis=-1, keepdims=True))).astype(BF16)
        attended = jnp.dot(weights, values, preferred_element_type=jnp.float32)
        outs[j][:, h * HEAD_WIDTH : (h + 1) * HEAD_WIDTH] = attended.astype(BF16)
        scores = following


def finish_kernel(head_rels, places, *refs):
    n_heads, n_pieces = len(head_rels), len(places)
    heads, pieces = refs[:n_heads], refs[n_heads : n_heads + n_pieces]
    gain, out, a_buf, w_buf, p_buf, w_sem = refs[n_heads + n_pieces :]
    copies = []
    for j, (row, rel, core, step) in enumerate(places):
        height, width = pieces[j].shape
        row_at = 0 if row is None else pl.multiple_of((lax.axis_index("dp") ^ row) * height, height)
        col_at = 0 if rel is None else pl.multiple_of(rank_of(rel, core) * width, width)
        copy = pltpu.make_async_copy(pieces[j], w_buf.at[pl.ds(row_at, height), pl.ds(col_at, width)], w_sem.at[j])
        copies.append((step, copy))
    copies.sort(key=lambda c: c[0])
    for _, copy in copies:
        copy.start()
    width = heads[0].shape[1]
    for j in range(n_heads):
        a_buf[:, pl.ds(pl.multiple_of(rank_of(head_rels[j]) * width, width), width)] = heads[j][...]
    rows, total = out.shape
    chunk = total // n_heads
    squares = jnp.zeros((rows, 1), jnp.float32)
    steps = [bin(j).count("1") for j in range(n_heads)]
    done = -1
    for rel, step in sorted(zip(range(n_heads), steps), key=lambda c: c[1]):
        for at, copy in copies:
            if done < at <= step:
                copy.wait()
        done = step
        cols = pl.ds(pl.multiple_of((lax.axis_index("sp") ^ rel) * chunk, chunk), chunk)
        projected = jnp.dot(a_buf[...], w_buf[:, cols], preferred_element_type=jnp.float32)
        squares = squares + jnp.sum(projected * projected, axis=-1, keepdims=True)
        p_buf[:, cols] = projected
    scale = lax.rsqrt(squares / total + EPS)
    out[...] = (p_buf[...] * scale * gain[...]).astype(BF16)


def rotation_table(length):
    quarter = HEAD_WIDTH // 4
    freq = THETA ** (-np.arange(quarter) / quarter)
    at = np.arange(length)
    row, col = (at // GRID_W)[:, None] * freq, (at % GRID_W)[:, None] * freq
    cosine = [np.cos(row), np.cos(row), np.cos(col), np.cos(col)]
    sine = [-np.sin(row), np.sin(row), -np.sin(col), np.sin(col)]
    return jnp.asarray(np.concatenate(cosine + sine, axis=1).astype(np.float32))


def on_device(tokens, in_gain, query_weight, key_weight, value_matrix, query_gain, key_gain, out_weight, out_gain):
    sequence = tokens[0]
    sp, dp = lax.axis_size("sp"), lax.axis_size("dp")
    rows, width = sequence.shape
    w_rows = query_weight.shape[0]
    heads = QUERY_HEAD_COUNT // sp
    kv = max(1, KEY_VALUE_HEADS // sp)
    q_width, kv_width, o_width = heads * HEAD_WIDTH, kv * HEAD_WIDTH, out_weight.shape[1] // sp
    all_width = q_width + 2 * kv_width
    even_rel, odd_rel = offsets(sp)
    rels = list(zip(even_rel, odd_rel))

    normed, cols, quarter = call(
        functools.partial(prepare_kernel, (q_width, kv_width, o_width, QUERY_HEAD_COUNT // KEY_VALUE_HEADS)),
        "prepare",
        (sequence, in_gain.reshape(1, -1), query_weight, key_weight, value_matrix, out_weight),
        [VMEM, VMEM, ANY, ANY, ANY, ANY],
        ((rows, width), (w_rows, all_width), (w_rows, o_width)),
        [DMA((4,))],
        rows * width * 10,
        16,
    )

    line_bits = [1 << i for i in range(dp.bit_length() - 2, -1, -1)]
    x_blocks = plane_gather(normed)
    w_blocks, w_rel = line_gather(cols, line_bits)

    if sp * dp > 64:
        pieces = [lax.all_gather(out_weight, "dp", axis=0, tiled=True)]
        places = [(None, None, 0, 0)]
    else:
        pieces = [out_weight, line_swap(out_weight, 1)]
        places = [(0, None, 0, 0), (1, None, 0, 0)]
        z_blocks, z_rel = line_gather(quarter, line_bits[:-1])
        for block, rel in list(zip(z_blocks, z_rel))[1:]:
            for j, piece in enumerate(plane_gather(block)):
                step = bin(j).count("1")
                pieces += [piece, line_swap(piece, 1)]
                places += [(rel, rels[j], 0, step), (rel ^ 1, rels[j], 1, step)]

    table = rotation_table(rows * sp)
    gains = jnp.stack([query_gain, key_gain])
    cut = sp // 2 + 1
    n = cut
    per_block = 2 * rows * width * all_width
    *first, weight = call(
        functools.partial(project_first_kernel, heads, kv, rels[:cut], w_rel),
        "project_first",
        (*x_blocks[:cut], *w_blocks, table, gains),
        [VMEM] * n + [ANY] * (dp + 1) + [VMEM],
        [(rows, q_width)] * n + [(rows, 2 * kv_width)] * n + [(width, all_width)],
        [pltpu.VMEM((n, rows, 2 * HEAD_WIDTH), jnp.float32), DMA((dp,)), DMA((n,))],
        n * per_block,
        20 + 2 * n,
    )
    queries, kvs = first[:n], first[n:]
    n = sp - cut
    if n:
        rest = call(
            functools.partial(project_rest_kernel, heads, kv, rels[cut:]),
            "project_rest",
            (*x_blocks[cut:], weight, table, gains),
            [VMEM] * n + [VMEM, ANY, VMEM],
            [(rows, q_width)] * n + [(rows, 2 * kv_width)] * n,
            [pltpu.VMEM((n, rows, 2 * HEAD_WIDTH), jnp.float32), DMA((n,))],
            n * per_block,
            20 + 2 * n,
        )
        queries, kvs = queries + list(rest[:n]), kvs + list(rest[n:])

    attended = [None] * sp
    for name, group in (("attend_others", range(1, sp)), ("attend_own", range(1))):
        results = call(
            functools.partial(attend_kernel, len(group), sp, heads, kv),
            name,
            (*[queries[j] for j in group], *kvs),
            [VMEM] * (len(group) + sp),
            [(rows, q_width)] * len(group),
            [pltpu.VMEM((rows * sp, 2 * kv_width), BF16)],
            4 * len(group) * rows * rows * sp * q_width,
            24,
        )
        for j, block in zip(group, results):
            attended[j] = plane_swap(block, even_rel[j], odd_rel[j]) if j else block

    (result,) = call(
        functools.partial(finish_kernel, rels, places),
        "finish",
        (*attended, *pieces, out_gain.reshape(1, -1)),
        [VMEM] * sp + [ANY] * len(pieces) + [VMEM],
        [(rows, width)],
        [
            pltpu.VMEM((rows, q_width * sp), BF16),
            pltpu.VMEM((q_width * sp, width), BF16),
            pltpu.VMEM((rows, width), jnp.float32),
            DMA((len(pieces),)),
        ],
        2 * rows * width * width,
        24,
    )
    return result[None]


def solution(mesh):
    placed = (
        P("dp", "sp", None),
        P(),
        P("dp", None),
        P("dp", None),
        P("dp", None),
        P(),
        P(),
        P("dp", None),
        P(),
    )
    return jax.shard_map(on_device, mesh=mesh, in_specs=placed, out_specs=P("dp", "sp", None), check_vma=False)
```
